32 devices in a mesh: grp: 2 (over y), fs: 4 (over z), tp: 4 (over x, core).
Axes of the slice: x: 2, y: 2, z: 4, core: 2. Of those that a mesh axis runs over, the one named last changes fastest.
Arguments:
- prompt: bfloat16 [8, 1024, 2048], P(('grp', 'tp')), parts along dimension 0, may hold values from -6 to 6
- gate_first: float32 [2048, 5632], P('fs', 'tp'), may hold values from -0.125 to 0.125
- up_first: float32 [2048, 5632], P('fs', 'tp'), may hold values from -0.125 to 0.125
- down_first: float32 [5632, 2048], P('fs', 'tp'), may hold values from -0.3125 to 0.3125
- norm_gain: float32 [2048], replicated, may hold values from 0.1 to 1.9
- gate_second: float32 [2048, 5632], P('fs', 'tp'), may hold values from -0.125 to 0.125
- up_second: float32 [2048, 5632], P('fs', 'tp'), may hold values from -0.125 to 0.125
- down_second: float32 [5632, 2048], P('fs', 'tp'), may hold values from -0.3125 to 0.3125
Outputs:
- result: bfloat16 [8, 1024, 2048], P(('grp', 'tp'), 'fs'), parts along dimension 0
- gate_one: bfloat16 [4096, 5632], P('grp', 'fs'), parts along dimension 0
- up_one: bfloat16 [4096, 5632], P('grp', 'fs'), parts along dimension 0
- down_one: bfloat16 [5632, 4096], P('fs', 'grp'), parts along dimension 1
- gate_two: bfloat16 [4096, 5632], P('grp', 'fs'), parts along dimension 0
- up_two: bfloat16 [4096, 5632], P('grp', 'fs'), parts along dimension 0
- down_two: bfloat16 [5632, 4096], P('fs', 'grp'), parts along dimension 1
The draws below stay inside these ranges and needn't reach their ends.
There are 2 independent parts, one for each index of `grp`. The reference program is written for one: setup_inputs(seed, part) draws one part's arguments, and reference() takes and returns one part's arrays. A program takes and returns all parts, laid end to end along the dimension named above; an argument that names none is the same for every part. Nothing has to cross between parts.
All inputs are finite; a program needn't handle non-finite values.
Results may differ from the reference program's by a relative error of at most 0.029.
Values may be sent and summed in bfloat16 or wider, within the bound.
A program may use at most 192 MiB of HBM per device.

```python
import jax
import jax.numpy as jnp
from jax import lax

D = 2048
FF = 5632
LENGTH = 1024
PROMPTS = 4
N_FS = 4


def block_levels(rng, shape, pieces, least, largest):
    factor_of = 1.0
    for axis_at, blocks in pieces:
        heights = jax.random.uniform(jax.random.fold_in(jax.random.fold_in(rng, 6), axis_at), (blocks,), jnp.float32, least / len(pieces), largest / len(pieces))
        factor_of = factor_of * jnp.repeat(jnp.exp(heights), shape[axis_at] // blocks).reshape((-1,) + (1,) * (len(shape) - 1 - axis_at))
    return factor_of


def bell_draw(key, extent, scale, bound, shards=(), kind=jnp.bfloat16):
    loudness = block_levels(key, extent, shards, -0.22, 0.18) if shards else 1.0
    entries = jax.random.normal(key, extent, jnp.float32) * scale * loudness
    return jnp.minimum(jnp.maximum(entries, -bound), bound).astype(kind)


def setup_inputs(seed: int = 0, part: int = 0) -> dict:
    seeds = jax.random.split(jax.random.key(seed), 9)
    part_keys = jax.random.split(jax.random.fold_in(seeds[8], part), 9)
    prompt = bell_draw(part_keys[0], (PROMPTS, LENGTH, D), 1.0, 6.0, ((0, 4),))
    gate_first = bell_draw(seeds[1], (D, FF), D ** -0.5, 0.125, ((0, 4), (1, 4)), jnp.float32)
    up_first = bell_draw(seeds[2], (D, FF), D ** -0.5, 0.125, ((0, 4), (1, 4)), jnp.float32)
    down_first = bell_draw(seeds[3], (FF, D), (4.0 * FF ** -0.5), 0.3125, ((0, 4), (1, 4)), jnp.float32)
    norm_gain = jnp.clip(1.0 + 0.18 * jax.random.normal(seeds[4], (D,), jnp.float32), 0.1, 1.9)
    gate_second = bell_draw(seeds[5], (D, FF), D ** -0.5, 0.125, ((0, 4), (1, 4)), jnp.float32)
    up_second = bell_draw(seeds[6], (D, FF), D ** -0.5, 0.125, ((0, 4), (1, 4)), jnp.float32)
    down_second = bell_draw(seeds[7], (FF, D), (4.0 * FF ** -0.5), 0.3125, ((0, 4), (1, 4)), jnp.float32)
    return dict(prompt=prompt, gate_first=gate_first, up_first=up_first, down_first=down_first, norm_gain=norm_gain, gate_second=gate_second, up_second=up_second, down_second=down_second)


norm_eps = 1e-05
deep_alpha = 2.0 ** 0.25
half_step = 0.5

def plain_norm(values):
    row_mean = lax.optimization_barrier(jnp.mean(values, axis=-1, keepdims=True))
    centred = values - row_mean
    variance = lax.optimization_barrier(jnp.mean(centred * centred, axis=-1, keepdims=True))
    return centred * lax.rsqrt(variance + norm_eps)

def gated_hidden(inputs, gate_proj, up_proj):
    gate_act = jnp.dot(inputs, gate_proj, preferred_element_type=jnp.float32)
    up_act = jnp.dot(inputs, up_proj, preferred_element_type=jnp.float32)
    return (jax.nn.silu(gate_act) * up_act).astype(jnp.bfloat16)

def block_sums(hidden, down_proj):
    block_width = hidden.shape[1] // N_FS

    def one_block(carried, block_index):
        hidden_block = lax.dynamic_slice_in_dim(hidden, block_index * block_width, block_width, 1)
        down_block = lax.dynamic_slice_in_dim(down_proj, block_index * block_width, block_width, 0)
        partial_term = jnp.dot(hidden_block, down_block, preferred_element_type=jnp.float32).astype(jnp.bfloat16)
        partial_term = lax.optimization_barrier(partial_term)
        return (carried + partial_term.astype(jnp.float32), None)
    start_sum = jnp.zeros((hidden.shape[0], down_proj.shape[1]), jnp.float32)
    summed, unused = lax.scan(one_block, start_sum, jnp.arange(N_FS, dtype=jnp.int32))
    return summed

def reference(prompt, gate_first, up_first, down_first, norm_gain, gate_second, up_second, down_second):
    gate_one = gate_first.astype(jnp.bfloat16)
    up_one = up_first.astype(jnp.bfloat16)
    down_one = down_first.astype(jnp.bfloat16)
    gate_two = (norm_gain[:, None] * gate_second).astype(jnp.bfloat16)
    up_two = (norm_gain[:, None] * up_second).astype(jnp.bfloat16)
    down_two = down_second.astype(jnp.bfloat16)
    tokens = prompt.reshape(-1, prompt.shape[-1])
    hidden_one = gated_hidden(tokens, gate_one, up_one)
    ffn_one = block_sums(hidden_one, down_one)
    normed_one = plain_norm(deep_alpha * tokens.astype(jnp.float32) + half_step * ffn_one).astype(jnp.bfloat16)
    hidden_two = gated_hidden(normed_one, gate_two, up_two)
    ffn_two = block_sums(hidden_two, down_two)
    residual_two = deep_alpha * norm_gain * normed_one.astype(jnp.float32)
    result = plain_norm(residual_two + half_step * ffn_two).astype(jnp.bfloat16).reshape(prompt.shape)
    return (result, gate_one, up_one, down_one, gate_two, up_two, down_two)
```

```python
import jax
import jax.numpy as jnp
from jax import lax
from jax.sharding import PartitionSpec as P

norm_eps = 1e-05
deep_alpha = 2.0**0.25
half_step = 0.5


def plain_norm(values):
    row_mean = jnp.mean(values, axis=-1, keepdims=True)
    centred = values - row_mean
    variance = jnp.mean(centred * centred, axis=-1, keepdims=True)
    return centred * lax.rsqrt(variance + norm_eps)


def gated_hidden(inputs, gate_proj, up_proj):
    gate_act = jnp.dot(inputs, gate_proj, preferred_element_type=jnp.float32)
    up_act = jnp.dot(inputs, up_proj, preferred_element_type=jnp.float32)
    return (jax.nn.silu(gate_act) * up_act).astype(jnp.bfloat16)


def relay_weights(gate_proj, up_proj, down_proj):
    gate_rows, up_rows, down_mine = (
        lax.all_gather(gate_proj, "tp", axis=1, tiled=True),
        lax.all_gather(up_proj, "tp", axis=1, tiled=True),
        lax.all_gather(down_proj, "tp", axis=1, tiled=True),
    )
    gate_mine, up_mine = (
        lax.all_to_all(gate_rows, "fs", split_axis=1, concat_axis=0, tiled=True),
        lax.all_to_all(up_rows, "fs", split_axis=1, concat_axis=0, tiled=True),
    )
    return (gate_mine, up_mine, down_mine)


def send_columns(gate_proj, up_proj):
    side, groups = lax.axis_size("tp"), lax.axis_size("grp")
    fs_index, grp_index, tp_index = (lax.axis_index(name) for name in ("fs", "grp", "tp"))
    rows, width = gate_proj.shape
    share = rows // (side * groups)
    held = jnp.zeros((side, 2, share, width), gate_proj.dtype)
    for turn in range(side):
        first = (lax.rem(fs_index + turn, side) * groups + grp_index) * share
        sent = jnp.stack(
            [
                lax.dynamic_slice_in_dim(gate_proj, first, share, 0),
                lax.dynamic_slice_in_dim(up_proj, first, share, 0),
            ]
        )
        pairs = [
            (f * side + t, t * side + (f + turn) % side)
            for f in range(side)
            for t in range(side)
        ]
        arrived = lax.ppermute(sent, ("fs", "tp"), pairs)
        source = lax.rem(tp_index + side - turn, side)
        held = lax.dynamic_update_slice_in_dim(held, arrived[None], source, 0)
    return held


def gather_columns(held):
    return lax.all_gather(held, ("grp", "tp"), axis=0)


def order_columns(gathered):
    side, groups = lax.axis_size("tp"), lax.axis_size("grp")
    share, width = gathered.shape[-2:]
    split = gathered.reshape(groups, side, side, 2, share, width)
    return tuple(
        split[:, :, :, which].transpose(2, 1, 0, 3, 4).reshape(-1, width) for which in range(2)
    )


def order_down(gathered):
    return gathered.transpose(1, 0, 2).reshape(gathered.shape[1], -1)


def ring(turn):
    count = lax.axis_size("fs")
    return [(f, (f + turn) % count) for f in range(count)]


def row_terms(hidden, down_proj):
    return jnp.dot(hidden, down_proj, preferred_element_type=jnp.float32)


def body(prompt, gate_first, up_first, down_first, norm_gain, gate_second, up_second, down_second):
    fs_index = lax.axis_index("fs")
    row_block = gate_first.shape[0]
    gain_rows = lax.dynamic_slice_in_dim(norm_gain, fs_index * row_block, row_block, 0)
    gate_a, up_a, down_a = (
        proj.astype(jnp.bfloat16) for proj in (gate_first, up_first, down_first)
    )
    gate_b = (gain_rows[:, None] * gate_second).astype(jnp.bfloat16)
    up_b = (gain_rows[:, None] * up_second).astype(jnp.bfloat16)
    down_b = down_second.astype(jnp.bfloat16)
    side, groups = lax.axis_size("tp"), lax.axis_size("grp")
    direct = lax.axis_size("fs") == side and row_block % (side * groups * 16) == 0
    if direct:
        down_gathered = lax.all_gather(down_a, "tp", axis=0)
        held, down_gathered = lax.optimization_barrier(
            (send_columns(gate_a, up_a), down_gathered)
        )
        gathered = gather_columns(held)
        gathered, gate_b, up_b, down_b = lax.optimization_barrier(
            (gathered, gate_b, up_b, down_b)
        )
        gate_one, up_one = order_columns(gathered)
        down_one = order_down(down_gathered)
        down_later = lax.all_gather(down_b, "tp", axis=0)
        later = gather_columns(send_columns(gate_b, up_b))
    else:
        gate_one, up_one, down_one = relay_weights(gate_a, up_a, down_a)
    tokens = prompt.reshape(-1, prompt.shape[-1])
    own_count = tokens.shape[0] // lax.axis_size("fs")
    own_first = fs_index * own_count
    fs_count = lax.axis_size("fs")

    def block_terms(rows, gate_proj, up_proj, down_proj):
        return row_terms(gated_hidden(rows, gate_proj, up_proj), down_proj).astype(jnp.bfloat16)

    def total_of(terms):
        total = terms[0].astype(jnp.float32)
        for term in terms[1:]:
            total = total + term.astype(jnp.float32)
        return total

    own_tokens = lax.dynamic_slice_in_dim(tokens, own_first, own_count, 0)
    turns = sorted(range(1, fs_count), key=lambda turn: -min(turn, fs_count - turn))
    terms_one = []
    for turn in turns:
        first = lax.rem(fs_index + turn, fs_count) * own_count
        rows = lax.dynamic_slice_in_dim(tokens, first, own_count, 0)
        terms_one.append(
            lax.ppermute(block_terms(rows, gate_one, up_one, down_one), "fs", ring(turn))
        )
    terms_one.append(block_terms(own_tokens, gate_one, up_one, down_one))
    if direct:
        later, down_later, terms_one[-1] = lax.optimization_barrier(
            (later, down_later, terms_one[-1])
        )
        gate_two, up_two = order_columns(later)
        down_two = order_down(down_later)
    else:
        gate_two, up_two, down_two = relay_weights(gate_b, up_b, down_b)
    normed_own = plain_norm(
        deep_alpha * own_tokens.astype(jnp.float32) + half_step * total_of(terms_one)
    ).astype(jnp.bfloat16)
    others = [(turn, lax.ppermute(normed_own, "fs", ring(turn))) for turn in turns]
    terms_two = [block_terms(normed_own, gate_two, up_two, down_two)]
    for turn, rows in others[1:] + others[:1]:
        terms_two.append(
            lax.ppermute(
                block_terms(rows, gate_two, up_two, down_two), "fs", ring(fs_count - turn)
            )
        )
    ffn_two = total_of(terms_two)
    residual_two = deep_alpha * norm_gain * normed_own.astype(jnp.float32)
    result = plain_norm(residual_two + half_step * ffn_two).astype(jnp.bfloat16)
    return (
        result.reshape(1, result.shape[0], result.shape[-1]),
        gate_one,
        up_one,
        down_one,
        gate_two,
        up_two,
        down_two,
    )


def solution(mesh):
    placed = (
        P(("grp", "tp"), None, None),
        P("fs", "tp"),
        P("fs", "tp"),
        P("fs", "tp"),
        P(),
        P("fs", "tp"),
        P("fs", "tp"),
        P("fs", "tp"),
    )
    return jax.shard_map(
        body,
        mesh=mesh,
        in_specs=placed,
        out_specs=(
            P(("grp", "tp"), "fs", None),
            P("grp", "fs"),
            P("grp", "fs"),
            P("fs", "grp"),
            P("grp", "fs"),
            P("grp", "fs"),
            P("fs", "grp"),
        ),
        check_vma=False,
    )
```
